1024 devices in a mesh: grp: 2 (over x), kv: 16 (over z), tp: 32 (over y, core).
Axes of the slice: x: 2, y: 16, z: 16, core: 2. Of those that a mesh axis runs over, the one named last changes fastest.
The devices are a block of a 4x16x16 slice.
Arguments:
- stream: bfloat16 [128, 4096], P('grp', ('kv', 'tp')), parts along dimension 0, may hold values from -6 to 6
- attn_gain: bfloat16 [4096], P('kv'), may hold values from 0.099609375 to 1.8984375
- mlp_gain: bfloat16 [4096], P('kv'), may hold values from 0.099609375 to 1.8984375
- w_query: bfloat16 [4096, 4096], P('kv', 'tp'), may hold values from -0.09375 to 0.09375
- w_key: bfloat16 [4096, 4096], P('kv', 'tp'), may hold values from -0.09375 to 0.09375
- w_value: bfloat16 [4096, 4096], P('kv', 'tp'), may hold values from -0.09375 to 0.09375
- w_zgate: bfloat16 [4096, 4096], P('kv', 'tp'), may hold values from -0.09375 to 0.09375
- w_decay: bfloat16 [4096, 32], P('kv'), may hold values from -0.09375 to 0.09375
- w_beta: bfloat16 [4096, 32], P('kv'), may hold values from -0.09375 to 0.09375
- decay_rate: float32 [32], P('tp'), may hold values from 0.03 to 3
- head_gain: float32 [128], replicated, may hold values from 0.1 to 1.9
- w_attn_out: bfloat16 [4096, 4096], P('tp', 'kv'), may hold values from -0.09375 to 0.09375
- w_gate: bfloat16 [4096, 11264], P('kv', 'tp'), may hold values from -0.09375 to 0.09375
- w_up: bfloat16 [4096, 11264], P('kv', 'tp'), may hold values from -0.09375 to 0.09375
- w_down: bfloat16 [11264, 4096], P('tp', 'kv'), may hold values from -0.0546875 to 0.0546875
- state: float32 [128, 32, 128, 128], P(('grp', 'kv'), 'tp'), parts along dimension 0, may hold values from -4 to 4
Outputs:
- next_stream: bfloat16 [128, 4096], P('grp', ('kv', 'tp')), parts along dimension 0
- new_state: float32 [128, 32, 128, 128], P(('grp', 'kv'), 'tp'), parts along dimension 0
The draws below stay inside these ranges and needn't reach their ends.
There are 2 independent parts, one for each index of `grp`. The reference program is written for one: setup_inputs(seed, part) draws one part's arguments, and reference() takes and returns one part's arrays. A program takes and returns all parts, laid end to end along the dimension named above; an argument that names none is the same for every part. Nothing has to cross between parts.
All inputs are finite; a program needn't handle non-finite values.
Results may differ from the reference program's by a relative error of at most 0.025.
Values may be sent and summed in bfloat16 or wider, within the bound.
A program may use at most 32 MiB of HBM per device.

```python
import math
import jax
import jax.numpy as jnp
from jax import lax

D = 4096
HEADS = 32
HEAD_DIM = 128
FF = 11264
BATCH = 64


def block_scale(rng, dims, pieces, least, top_value):
    level = 1.0
    for axis_at, parts in pieces:
        steps = jax.random.uniform(jax.random.fold_in(jax.random.fold_in(rng, 6), axis_at), (parts,), jnp.float32, least / len(pieces), top_value / len(pieces))
        level = level * jnp.repeat(jnp.exp(steps), dims[axis_at] // parts).reshape((-1,) + (1,) * (len(dims) - 1 - axis_at))
    return level


def centred(rng, extent, width, bound, split=(), dtype=jnp.bfloat16):
    result = width * jax.random.normal(rng, extent, jnp.float32)
    if split:
        result = result * block_scale(rng, extent, split, -0.22, 0.18)
    return jnp.clip(result, -bound, bound).astype(dtype)


def setup_inputs(seed: int = 0, part: int = 0) -> dict:
    seeds = jax.random.split(jax.random.key(seed), 17)
    own_keys = jax.random.split(jax.random.fold_in(seeds[16], part), 17)
    return {
        "stream": centred(own_keys[0], (BATCH, D), 1.0, 6.0, ((1, 512),)),
        "attn_gain": jnp.clip(1.0 + 0.18 * jax.random.normal(seeds[1], (D,), jnp.float32), 0.099609375, 1.8984375).astype(jnp.bfloat16),
        "mlp_gain": jnp.clip(1.0 + 0.18 * jax.random.normal(seeds[2], (D,), jnp.float32), 0.099609375, 1.8984375).astype(jnp.bfloat16),
        "w_query": centred(seeds[3], (D, HEADS * HEAD_DIM), D ** -0.5, 0.09375, ((0, 16), (1, 32))),
        "w_key": centred(seeds[4], (D, HEADS * HEAD_DIM), D ** -0.5, 0.09375, ((0, 16), (1, 32))),
        "w_value": centred(seeds[5], (D, HEADS * HEAD_DIM), D ** -0.5, 0.09375, ((0, 16), (1, 32))),
        "w_zgate": centred(seeds[6], (D, HEADS * HEAD_DIM), D ** -0.5, 0.09375, ((0, 16), (1, 32))),
        "w_decay": centred(seeds[7], (D, HEADS), D ** -0.5, 0.09375, ((0, 16),)),
        "w_beta": centred(seeds[8], (D, HEADS), D ** -0.5, 0.09375, ((0, 16),)),
        "decay_rate": jnp.clip(jnp.exp(math.log(3.0) - 4.6051702 * jax.random.uniform(seeds[9], (HEADS,), jnp.float32) ** block_scale(seeds[9], (HEADS,), ((0, 32),), -0.2, 0.2)), 0.03, 3.0),
        "head_gain": jnp.clip(1.0 + 0.18 * jax.random.normal(seeds[10], (HEAD_DIM,), jnp.float32), 0.1, 1.9),
        "w_attn_out": centred(seeds[11], (HEADS * HEAD_DIM, D), (HEADS * HEAD_DIM) ** -0.5, 0.09375, ((0, 32), (1, 16))),
        "w_gate": centred(seeds[12], (D, FF), D ** -0.5, 0.09375, ((0, 16), (1, 32))),
        "w_up": centred(seeds[13], (D, FF), D ** -0.5, 0.09375, ((0, 16), (1, 32))),
        "w_down": centred(seeds[14], (FF, D), FF ** -0.5, 0.0546875, ((0, 32), (1, 16))),
        "state": centred(own_keys[15], (BATCH, HEADS, HEAD_DIM, HEAD_DIM), 0.3, 4.0, ((0, 16), (1, 32)), jnp.float32),
    }


EPSILON = 1e-06

def l2_unit(values):
    return values * lax.rsqrt(lax.optimization_barrier(jnp.sum(values * values, axis=-1, keepdims=True)) + EPSILON)

def delta_update(query, key_vec, value_vec, log_decay, beta_gate, state):
    decayed = jnp.exp(log_decay)[..., None, None] * state
    recalled = jnp.einsum('shkv,shk->shv', decayed, key_vec, precision=lax.Precision.HIGHEST)
    update = beta_gate[..., None] * (value_vec - recalled)
    new_state = decayed + key_vec[..., :, None] * update[..., None, :]
    head_out = jnp.einsum('shkv,shk->shv', new_state, query, precision=lax.Precision.HIGHEST)
    return (new_state, head_out)

def head_mix(head_out, head_gain, z_gate):
    scaled = head_out * lax.rsqrt(lax.optimization_barrier(jnp.mean(head_out * head_out, axis=-1, keepdims=True)) + EPSILON)
    return (scaled * head_gain.astype(jnp.float32) * jax.nn.silu(z_gate)).astype(jnp.bfloat16)

def reference(stream, attn_gain, mlp_gain, w_query, w_key, w_value, w_zgate, w_decay, w_beta, decay_rate, head_gain, w_attn_out, w_gate, w_up, w_down, state):
    batch = stream.shape[0]
    stream_f = stream.astype(jnp.float32)
    row_scale = lax.rsqrt(lax.optimization_barrier(jnp.mean(stream_f * stream_f, axis=1, keepdims=True)) + EPSILON)
    normed = (stream_f * attn_gain.astype(jnp.float32)[None, :]).astype(jnp.bfloat16)

    def project(weight):
        return jnp.dot(normed, weight, preferred_element_type=jnp.float32) * row_scale
    query = l2_unit(project(w_query).reshape(batch, HEADS, HEAD_DIM)) * HEAD_DIM ** (-0.5)
    key_vec = l2_unit(project(w_key).reshape(batch, HEADS, HEAD_DIM))
    value_vec = project(w_value).reshape(batch, HEADS, HEAD_DIM)
    z_gate = project(w_zgate).reshape(batch, HEADS, HEAD_DIM)
    log_decay = -decay_rate[None, :] * jax.nn.softplus(project(w_decay))
    beta_gate = jax.nn.sigmoid(project(w_beta))
    new_state, head_out = delta_update(query, key_vec, value_vec, log_decay, beta_gate, state)
    mixed = head_mix(head_out, head_gain, z_gate).reshape(batch, HEADS * HEAD_DIM)
    residual_stream = (stream_f + jnp.dot(mixed, w_attn_out, preferred_element_type=jnp.float32)).astype(jnp.bfloat16)
    resid_f = residual_stream.astype(jnp.float32)
    mlp_scale = lax.rsqrt(lax.optimization_barrier(jnp.mean(resid_f * resid_f, axis=1, keepdims=True)) + EPSILON)
    normed_mlp = (resid_f * mlp_gain.astype(jnp.float32)[None, :]).astype(jnp.bfloat16)
    gate = jnp.dot(normed_mlp, w_gate, preferred_element_type=jnp.float32) * mlp_scale
    up_proj = jnp.dot(normed_mlp, w_up, preferred_element_type=jnp.float32) * mlp_scale
    hidden = (jax.nn.silu(gate) * up_proj).astype(jnp.bfloat16)
    next_stream = (resid_f + jnp.dot(hidden, w_down, preferred_element_type=jnp.float32)).astype(jnp.bfloat16)
    return (next_stream, new_state)
```

```python
import functools

import jax
import jax.numpy as jnp
from jax import lax
from jax.experimental import pallas as pl
from jax.experimental.pallas import tpu as pltpu
from jax.sharding import PartitionSpec as P

EPSILON = 1e-06
LANES = 128
MESH = pl.DeviceIdType.MESH
F32 = jnp.float32
BF16 = jnp.bfloat16


def fan_out(axis, peers, me, source, target, send_sem, recv_sem):
    half = peers // 2

    def to_offset(offset):
        peer = lax.rem(me + offset, peers)
        pltpu.make_async_remote_copy(
            src_ref=source(peer),
            dst_ref=target,
            send_sem=send_sem,
            recv_sem=recv_sem,
            device_id={axis: peer},
            device_id_type=MESH,
        ).start()

    def pair(step, carry):
        to_offset(half + step)
        to_offset(half - 1 - step)
        return carry

    lax.fori_loop(0, half - 1, pair, None)
    to_offset(peers - 1)


def wait_bytes(slots, sem):
    part = slots.at[pl.ds(0, slots.shape[0] - 1)]
    pltpu.make_async_copy(part, part, sem).wait()


def greet(axis, peers, me, barrier):
    def one(offset, carry):
        peer = lax.rem(me + offset, peers)
        pl.semaphore_signal(barrier, inc=1, device_id={axis: peer}, device_id_type=MESH)
        return carry

    lax.fori_loop(1, peers, one, None)


def silu(values):
    return values * jax.nn.sigmoid(values)


def dot(left, right):
    return jnp.dot(left, right, preferred_element_type=F32)


def dot_rows(left, right):
    return lax.dot_general(left, right, (((1,), (1,)), ((), ())), preferred_element_type=F32)


def merge_rows(slots):
    count = slots.shape[0]
    return jnp.concatenate([slots[at].astype(F32) for at in range(count)], axis=0).astype(BF16)


def layer(
    kv_peers,
    tp_peers,
    stream_ref,
    attn_gain_ref,
    mlp_gain_ref,
    decay_rate_ref,
    head_gain_ref,
    w_query_ref,
    w_key_ref,
    w_value_ref,
    w_zgate_ref,
    w_decay_ref,
    w_beta_ref,
    w_attn_out_ref,
    w_gate_ref,
    w_up_ref,
    w_down_ref,
    state_ref,
    next_ref,
    new_state_ref,
    w_mix,
    w_small,
    w_out,
    w_hidden,
    w_down,
    state,
    new_state,
    gathered,
    mix_send,
    mix_recv,
    head_slots,
    out_send,
    out_recv,
    resid_slots,
    hidden_send,
    hidden_recv,
    hidden_slots,
    down_send,
    down_recv,
    load_sems,
    state_sem,
    send_sems,
    recv_sems,
):
    kv = lax.axis_index("kv")
    tp = lax.axis_index("tp")
    batch = stream_ref.shape[1]
    rows = gathered.shape[0] * gathered.shape[1]
    features = kv_peers * rows
    seqs = state.shape[0]
    head_dim = state.shape[1]
    ff = w_gate_ref.shape[0]
    ff_pad = w_hidden.shape[0] // 2

    loads = [
        pltpu.make_async_copy(ref, w_mix.at[:, pl.ds(at * head_dim, head_dim)], load_sems.at[at])
        for at, ref in enumerate((w_query_ref, w_key_ref, w_value_ref, w_zgate_ref))
    ]
    loads += [
        pltpu.make_async_copy(w_decay_ref, w_small.at[0], load_sems.at[4]),
        pltpu.make_async_copy(w_beta_ref, w_small.at[1], load_sems.at[5]),
        pltpu.make_async_copy(w_attn_out_ref, w_out, load_sems.at[6]),
        pltpu.make_async_copy(w_gate_ref, w_hidden.at[pl.ds(0, ff)], load_sems.at[7]),
        pltpu.make_async_copy(w_up_ref, w_hidden.at[pl.ds(ff_pad, ff)], load_sems.at[8]),
        pltpu.make_async_copy(w_down_ref, w_down.at[pl.ds(0, ff)], load_sems.at[9]),
        pltpu.make_async_copy(state_ref, state, load_sems.at[10]),
    ]
    for load in loads:
        load.start()

    barrier = pltpu.get_barrier_semaphore()
    greet("tp", tp_peers, tp, barrier)
    greet("kv", kv_peers, kv, barrier)

    own = stream_ref[...].astype(F32)
    gathered[tp] = stream_ref[...]

    pl.semaphore_wait(barrier, tp_peers + kv_peers - 2)
    fan_out(
        "tp", tp_peers, tp, lambda peer: gathered.at[tp], gathered.at[tp], send_sems.at[0], recv_sems.at[0]
    )

    for load in loads:
        load.wait()
    heads = w_small.shape[1]
    is_own = lax.broadcasted_iota(jnp.int32, (heads, rows), 0) == tp
    own_decay = jnp.sum(jnp.where(is_own, w_small[0].astype(F32), 0.0), axis=0, keepdims=True)
    own_beta = jnp.sum(jnp.where(is_own, w_small[1].astype(F32), 0.0), axis=0, keepdims=True)
    small_row = lax.broadcasted_iota(jnp.int32, (LANES, rows), 0)
    small = jnp.where(small_row == 0, own_decay, jnp.where(small_row == 1, own_beta, 0.0))
    w_mix[:, pl.ds(4 * head_dim, LANES)] = small.T.astype(BF16)
    blank = jnp.zeros((ff_pad - ff, rows), BF16)
    w_hidden[pl.ds(ff, ff_pad - ff)] = blank
    w_hidden[pl.ds(ff_pad + ff, ff_pad - ff)] = blank
    w_down[pl.ds(ff, ff_pad - ff)] = jnp.zeros((ff_pad - ff, w_down.shape[1]), BF16)

    def normed_block(slots, gain_ref):
        block = slots[...].astype(F32).reshape(rows, batch).T
        squares = jnp.sum(block * block, axis=1, keepdims=True)
        gain = gain_ref[...].astype(F32).reshape(1, rows)
        return (block * gain).astype(BF16), squares

    def by_sequence(values, send, recv, phase):
        for at in range(kv_peers):
            send[at] = values[at * seqs : (at + 1) * seqs].astype(BF16)
        recv[kv] = send[kv]
        fan_out(
            "kv", kv_peers, kv, lambda peer: send.at[peer], recv.at[kv], send_sems.at[phase], recv_sems.at[phase]
        )

    def by_feature(values, send, recv, phase):
        send[...] = values.T.reshape(send.shape).astype(BF16)
        recv[tp] = send[tp]
        fan_out(
            "tp", tp_peers, tp, lambda peer: send.at[peer], recv.at[tp], send_sems.at[phase], recv_sems.at[phase]
        )

    def summed(recv, phase):
        wait_bytes(recv, recv_sems.at[phase])
        return jnp.sum(recv[...].astype(F32), axis=0)

    wait_bytes(gathered, recv_sems.at[0])
    normed, squares = normed_block(gathered, attn_gain_ref)
    pieces = dot(normed, w_mix[...])
    piece_lane = lax.broadcasted_iota(jnp.int32, pieces.shape, 1)
    pieces = jnp.where(piece_lane == 4 * head_dim + 2, squares, pieces)
    by_sequence(pieces, mix_send, mix_recv, 1)

    mix = summed(mix_recv, 1)
    small_at = 4 * head_dim
    scale = lax.rsqrt(mix[:, small_at + 2 : small_at + 3] / features + EPSILON)
    query_raw = mix[:, 0:head_dim] * scale
    key_raw = mix[:, head_dim : 2 * head_dim] * scale
    value_vec = mix[:, 2 * head_dim : 3 * head_dim] * scale
    z_gate = mix[:, 3 * head_dim : 4 * head_dim] * scale
    decay_pre = mix[:, small_at : small_at + 1] * scale
    beta_gate = jax.nn.sigmoid(mix[:, small_at + 1 : small_at + 2] * scale)

    def unit(values):
        return values * lax.rsqrt(jnp.sum(values * values, axis=1, keepdims=True) + EPSILON)

    query = unit(query_raw) * head_dim ** (-0.5)
    key_vec = unit(key_raw)
    softplus = jnp.maximum(decay_pre, 0.0) + jnp.log1p(jnp.exp(-jnp.abs(decay_pre)))
    decay = jnp.exp(-decay_rate_ref[0] * softplus)
    columns = jnp.concatenate([key_vec, query], axis=0).T
    recalled = []
    looked_up = []
    for at in range(seqs):
        one = state[at]
        recalled.append(jnp.sum(one * columns[:, at : at + 1], axis=0, keepdims=True))
        looked_up.append(jnp.sum(one * columns[:, seqs + at : seqs + at + 1], axis=0, keepdims=True))
    recalled = jnp.concatenate(recalled, axis=0) * decay
    looked_up = jnp.concatenate(looked_up, axis=0) * decay
    update = beta_gate * (value_vec - recalled)
    head_out = looked_up + update * jnp.sum(key_vec * query, axis=1, keepdims=True)
    head_gain = head_gain_ref[...].reshape(1, head_dim)
    mixed = head_out * lax.rsqrt(jnp.mean(head_out * head_out, axis=1, keepdims=True) + EPSILON)
    mixed = (mixed * head_gain * silu(z_gate)).astype(BF16)
    head_slots[kv] = mixed
    fan_out(
        "kv", kv_peers, kv, lambda peer: head_slots.at[kv], head_slots.at[kv], send_sems.at[2], recv_sems.at[2]
    )

    for at in range(seqs):
        new_state[at] = decay[at : at + 1] * state[at] + columns[:, at : at + 1] * update[at : at + 1]
    state_out = pltpu.make_async_copy(new_state, new_state_ref, state_sem)
    state_out.start()

    wait_bytes(head_slots, recv_sems.at[2])
    attn = dot(merge_rows(head_slots), w_out[...])
    by_feature(attn, out_send, out_recv, 3)
    residual = (own + summed(out_recv, 3)).astype(BF16)
    resid_slots[tp] = residual
    fan_out(
        "tp", tp_peers, tp, lambda peer: resid_slots.at[tp], resid_slots.at[tp], send_sems.at[4], recv_sems.at[4]
    )

    wait_bytes(resid_slots, recv_sems.at[4])
    normed, squares = normed_block(resid_slots, mlp_gain_ref)
    pieces = dot_rows(normed, w_hidden[...])
    piece_lane = lax.broadcasted_iota(jnp.int32, pieces.shape, 1)
    pieces = jnp.where(piece_lane == ff, squares, pieces)
    by_sequence(pieces, hidden_send, hidden_recv, 5)

    both = summed(hidden_recv, 5)
    scale = lax.rsqrt(both[:, ff : ff + 1] / features + EPSILON)
    hidden = silu(both[:, :ff_pad] * scale) * (both[:, ff_pad:] * scale)
    hidden_slots[kv] = hidden.astype(BF16)
    fan_out(
        "kv", kv_peers, kv, lambda peer: hidden_slots.at[kv], hidden_slots.at[kv], send_sems.at[6], recv_sems.at[6]
    )

    wait_bytes(hidden_slots, recv_sems.at[6])
    down = dot(merge_rows(hidden_slots), w_down[...])
    by_feature(down, down_send, down_recv, 7)
    next_ref[...] = (residual.astype(F32) + summed(down_recv, 7)).astype(BF16)

    for phase, slots in enumerate(
        (gathered, mix_send, head_slots, out_send, resid_slots, hidden_send, hidden_slots, down_send)
    ):
        wait_bytes(slots, send_sems.at[phase])
    state_out.wait()


def local(
    kv_peers,
    tp_peers,
    stream,
    attn_gain,
    mlp_gain,
    w_query,
    w_key,
    w_value,
    w_zgate,
    w_decay,
    w_beta,
    decay_rate,
    head_gain,
    w_attn_out,
    w_gate,
    w_up,
    w_down,
    state,
):
    batch, width = stream.shape
    rows, head_dim = w_query.shape
    seqs = state.shape[0]
    heads = w_decay.shape[1]
    ff = w_gate.shape[1]
    ff_pad = pl.cdiv(ff + 1, LANES) * LANES
    vmem = pl.BlockSpec(memory_space=pltpu.VMEM)
    smem = pl.BlockSpec(memory_space=pltpu.SMEM)
    hbm = pl.BlockSpec(memory_space=pl.ANY)
    feature_slots = pltpu.VMEM((tp_peers, width, batch), BF16)
    mix_slots = pltpu.VMEM((kv_peers, seqs, 4 * head_dim + LANES), BF16)
    hidden_slots = pltpu.VMEM((kv_peers, seqs, 2 * ff_pad), BF16)
    next_stream, new_state = pl.pallas_call(
        functools.partial(layer, kv_peers, tp_peers),
        name="layer",
        out_shape=(
            jax.ShapeDtypeStruct((width, batch), BF16),
            jax.ShapeDtypeStruct((seqs, head_dim, head_dim), F32),
        ),
        in_specs=[vmem, vmem, vmem, smem, vmem] + [hbm] * 11,
        out_specs=(vmem, hbm),
        scratch_shapes=[
            pltpu.VMEM((rows, 4 * head_dim + LANES), BF16),
            pltpu.VMEM((2, heads, rows), BF16),
            pltpu.VMEM((head_dim, w_attn_out.shape[1]), BF16),
            pltpu.VMEM((2 * ff_pad, rows), BF16),
            pltpu.VMEM((ff_pad, w_down.shape[1]), BF16),
            pltpu.VMEM((seqs, head_dim, head_dim), F32),
            pltpu.VMEM((seqs, head_dim, head_dim), F32),
            feature_slots,
            mix_slots,
            mix_slots,
            pltpu.VMEM((kv_peers, seqs, head_dim), BF16),
            feature_slots,
            feature_slots,
            feature_slots,
            hidden_slots,
            hidden_slots,
            pltpu.VMEM((kv_peers, seqs, ff_pad), BF16),
            feature_slots,
            feature_slots,
            pltpu.SemaphoreType.DMA((11,)),
            pltpu.SemaphoreType.DMA,
            pltpu.SemaphoreType.DMA((8,)),
            pltpu.SemaphoreType.DMA((8,)),
        ],
        compiler_params=pltpu.CompilerParams(collective_id=0, has_side_effects=True),
    )(
        stream.T,
        attn_gain,
        mlp_gain,
        decay_rate,
        head_gain,
        w_query,
        w_key,
        w_value,
        w_zgate,
        w_decay.T,
        w_beta.T,
        w_attn_out,
        w_gate.T,
        w_up.T,
        w_down,
        state.reshape(seqs, head_dim, head_dim),
    )
    return next_stream.T, new_state.reshape(state.shape)


def solution(mesh):
    return jax.shard_map(
        functools.partial(local, mesh.shape["kv"], mesh.shape["tp"]),
        mesh=mesh,
        in_specs=(
            P("grp", ("kv", "tp")),
            P("kv"),
            P("kv"),
            P("kv", "tp"),
            P("kv", "tp"),
            P("kv", "tp"),
            P("kv", "tp"),
            P("kv", None),
            P("kv", None),
            P("tp"),
            P(),
            P("tp", "kv"),
            P("kv", "tp"),
            P("kv", "tp"),
            P("tp", "kv"),
            P(("grp", "kv"), "tp", None, None),
        ),
        out_specs=(P("grp", ("kv", "tp")), P(("grp", "kv"), "tp", None, None)),
        check_vma=False,
    )
```

```python
import functools

import jax
import jax.numpy as jnp
from jax import lax
from jax.experimental import pallas as pl
from jax.experimental.pallas import tpu as pltpu
from jax.sharding import PartitionSpec as P

EPSILON = 1e-06
LANES = 128
REPEATS = 4
MESH = pl.DeviceIdType.MESH
F32 = jnp.float32
BF16 = jnp.bfloat16


def start_copy(axis, peer, source, target, send_sem, recv_sem):
    pltpu.make_async_remote_copy(
        src_ref=source,
        dst_ref=target,
        send_sem=send_sem,
        recv_sem=recv_sem,
        device_id={axis: peer},
        device_id_type=MESH,
    ).start()


def far_first(peers, me, visit):
    half = peers // 2

    def pair(step, carry):
        visit(lax.rem(me + half + step, peers))
        visit(lax.rem(me + half - 1 - step, peers))
        return carry

    lax.fori_loop(0, half - 1, pair, None)
    visit(lax.rem(me + peers - 1, peers))


def wait_bytes(slots, count, sem):
    part = slots.at[pl.ds(0, count)]
    pltpu.make_async_copy(part, part, sem).wait()


def silu(values):
    return values * jax.nn.sigmoid(values)


def dot(left, right):
    return jnp.dot(left, right, preferred_element_type=F32)


def dot_rows(left, right):
    return lax.dot_general(left, right, (((1,), (1,)), ((), ())), preferred_element_type=F32)


def merge_rows(slots):
    count = slots.shape[0]
    return jnp.concatenate([slots[at].astype(F32) for at in range(count)], axis=0).astype(BF16)


def layer(
    kv_peers,
    tp_peers,
    stream_ref,
    attn_gain_ref,
    mlp_gain_ref,
    decay_rate_ref,
    head_gain_ref,
    w_query_ref,
    w_key_ref,
    w_value_ref,
    w_zgate_ref,
    w_decay_ref,
    w_beta_ref,
    w_attn_out_ref,
    w_gate_ref,
    w_up_ref,
    w_down_ref,
    state_ref,
    next_ref,
    new_state_ref,
    attn_gain,
    mlp_gain,
    decay_rate,
    head_gain,
    w_mix,
    w_small,
    w_out,
    w_hidden,
    w_down,
    w_down_split,
    state,
    own_folded,
    resid_folded,
    gathered,
    mix_send,
    mix_recv,
    head_slots,
    out_send,
    out_recv,
    resid_slots,
    hidden_send,
    hidden_recv,
    hidden_slots,
    down_send,
    down_recv,
    stream_sem,
    slot_sems,
    load_sems,
    ready_sems,
    row_ready_sems,
    send_sems,
    recv_sems,
):
    kv = lax.axis_index("kv")
    tp = lax.axis_index("tp")
    width, batch = stream_ref.shape
    rows = gathered.shape[0] * gathered.shape[1]
    fold = rows // 2
    features = kv_peers * rows
    seqs = state.shape[0]
    head_dim = state.shape[1]
    ff = w_gate_ref.shape[0]
    ff_pad = w_hidden.shape[0] // 2
    chips = tp_peers // 2
    chip = tp // 2
    core = lax.rem(tp, 2)
    near = chips // 4
    pieces_count = out_send.shape[0]
    window = pieces_count // 2

    def on_chip(offset, which):
        return lax.rem(2 * (chip + chips + offset), tp_peers) + which

    def near_peers(visit):
        def ring(step, carry):
            for which in (0, 1):
                visit(on_chip(near - step, which))
                visit(on_chip(step - near, which))
            return carry

        lax.fori_loop(0, near, ring, None)
        visit(on_chip(0, 1 - core))

    barrier = pltpu.get_barrier_semaphore()

    def say(axis, sem):
        def one(peer):
            pl.semaphore_signal(sem, inc=1, device_id={axis: peer}, device_id_type=MESH)

        return one

    def loop(start, stop, visit):
        def step(at, carry):
            visit(at)
            return carry

        lax.fori_loop(start, stop, step, None)

    own_slot = pltpu.make_async_copy(stream_ref, gathered.at[tp], stream_sem)
    own_slot.start()

    rank = lax.rem(kv + kv_peers - 1, kv_peers)

    def at_rank(which):
        return lax.rem(which + 1, kv_peers)

    def row_rank(which):
        return lax.rem(which + tp_peers - 1, tp_peers)

    own_row_rank = row_rank(tp)

    def above(visit):
        def one(peer):
            @pl.when(row_rank(peer) > own_row_rank)
            def _():
                visit(peer)

        return one

    def below(visit):
        def one(peer):
            @pl.when(row_rank(peer) < own_row_rank)
            def _():
                visit(peer)

        return one

    with jax.named_scope("greet"):
        near_peers(above(say("tp", barrier)))
        loop(rank + 1, kv_peers, lambda which: say("kv", barrier)(at_rank(which)))
    with jax.named_scope("barrier"):
        expected = rank
        for step in range(near):
            for which in (0, 1):
                for peer in (on_chip(near - step, which), on_chip(step - near, which)):
                    expected += jnp.where(row_rank(peer) < own_row_rank, 1, 0)
        expected += jnp.where(row_rank(on_chip(0, 1 - core)) < own_row_rank, 1, 0)

        @pl.when(expected > 0)
        def _():
            pl.semaphore_wait(barrier, expected)

        own_slot.wait()

    def send_slot(slot, peer, send_sem):
        start_copy("tp", peer, gathered.at[slot], gathered.at[slot], send_sem, slot_sems.at[slot])

    def wait_slot(slot):
        pltpu.make_async_copy(gathered.at[slot], gathered.at[slot], slot_sems.at[slot]).wait()

    def answer(peer):
        say("tp", row_ready_sems.at[tp])(peer)
        send_slot(tp, peer, send_sems.at[0])

    def follow(peer):
        pl.semaphore_wait(row_ready_sems.at[peer], 1)
        send_slot(tp, peer, send_sems.at[0])

    with jax.named_scope("fan_near"):
        near_peers(below(answer))
        loop(0, rank, lambda which: say("kv", ready_sems.at[kv])(at_rank(which)))

    loads = [
        pltpu.make_async_copy(ref, w_mix.at[:, pl.ds(at * head_dim, head_dim)], load_sems.at[at])
        for at, ref in enumerate((w_query_ref, w_key_ref, w_value_ref, w_zgate_ref))
    ]
    loads += [
        pltpu.make_async_copy(w_decay_ref, w_small.at[0], load_sems.at[4]),
        pltpu.make_async_copy(w_beta_ref, w_small.at[1], load_sems.at[5]),
        pltpu.make_async_copy(attn_gain_ref, attn_gain, load_sems.at[6]),
        pltpu.make_async_copy(state_ref, state, load_sems.at[7]),
        pltpu.make_async_copy(decay_rate_ref, decay_rate, load_sems.at[8]),
        pltpu.make_async_copy(head_gain_ref, head_gain, load_sems.at[9]),
        pltpu.make_async_copy(w_attn_out_ref, w_out, load_sems.at[10]),
        pltpu.make_async_copy(mlp_gain_ref, mlp_gain, load_sems.at[11]),
        pltpu.make_async_copy(w_gate_ref, w_hidden.at[pl.ds(0, ff)], load_sems.at[12]),
        pltpu.make_async_copy(w_up_ref, w_hidden.at[pl.ds(ff_pad, ff)], load_sems.at[13]),
        pltpu.make_async_copy(w_down_ref, w_down.at[pl.ds(0, ff)], load_sems.at[14]),
    ]
    for load in loads:
        load.start()

    with jax.named_scope("follow"):
        near_peers(above(follow))

    def relay(offset, to_chip):
        for which in (0, 1):
            slot = on_chip(offset, which)
            wait_slot(slot)
            send_slot(slot, on_chip(to_chip, core), send_sems.at[8])

    with jax.named_scope("relay"):
        loop(1, near, lambda offset: relay(-offset, near))
        loop(1, near + 1, lambda offset: relay(offset, -near))

    with jax.named_scope("loads"):
        for load in loads:
            load.wait()
    heads = w_small.shape[1]
    is_own = lax.broadcasted_iota(jnp.int32, (heads, rows), 0) == tp
    own_decay = jnp.sum(jnp.where(is_own, w_small[0].astype(F32), 0.0), axis=0, keepdims=True)
    own_beta = jnp.sum(jnp.where(is_own, w_small[1].astype(F32), 0.0), axis=0, keepdims=True)
    small_row = lax.broadcasted_iota(jnp.int32, (LANES, rows), 0)
    small = jnp.where(small_row == 0, own_decay, jnp.where(small_row == 1, own_beta, 0.0))
    w_mix[:, pl.ds(4 * head_dim, LANES)] = small.T.astype(BF16)
    blank = jnp.zeros((ff_pad - ff, rows), BF16)
    w_hidden[pl.ds(ff, ff_pad - ff)] = blank
    w_hidden[pl.ds(ff_pad + ff, ff_pad - ff)] = blank
    w_down[pl.ds(ff, ff_pad - ff)] = jnp.zeros((ff_pad - ff, rows), BF16)
    from_at = lax.broadcasted_iota(jnp.int32, (rows, rows), 0)
    to_at = lax.broadcasted_iota(jnp.int32, (rows, rows), 1)
    part = width // 2
    to_low = lax.rem(to_at, fold)
    wanted = (to_low // part) * width + lax.rem(to_low, part) + jnp.where(to_at >= fold, part, 0)
    w_down_split[...] = dot(w_down[...], (from_at == wanted).astype(BF16)).astype(BF16)

    def folded(values):
        return jnp.concatenate([values[:, :fold], values[:, fold:]], axis=0).T

    def unfolded(values):
        values = values.T
        return jnp.concatenate([values[:batch], values[batch:]], axis=1)

    def normed_block(block, gain):
        squares = jnp.sum(block * block, axis=1, keepdims=True)
        return (block * gain[...].astype(F32).reshape(1, rows)).astype(BF16), squares

    def to_sequences(values, send, recv):
        for at in range(kv_peers):
            send[at] = values[at * seqs : (at + 1) * seqs].astype(BF16)
        recv[kv] = send[kv]

    def summed(slots):
        return jnp.sum(slots[...].astype(F32), axis=0)

    def copy_to(axis, source, target, phase):
        def one(peer):
            start_copy(axis, peer, source(peer), target, send_sems.at[phase], recv_sems.at[phase])

        return one

    with jax.named_scope("relay_wait"):
        wait_slot(on_chip(0, 1 - core))

        def from_chip(offset):
            wait_slot(on_chip(offset, 0))
            wait_slot(on_chip(offset, 1))

        from_chip(-near)
        loop(near + 1, chips - near, from_chip)
    block = gathered[...].astype(F32).reshape(rows, batch).T
    normed, squares = normed_block(block, attn_gain)
    pieces = dot(normed, w_mix[...])
    piece_lane = lax.broadcasted_iota(jnp.int32, pieces.shape, 1)
    pieces = jnp.where(piece_lane == 4 * head_dim + 2, squares, pieces)
    to_sequences(pieces, mix_send, mix_recv)
    send_mix = copy_to("kv", lambda peer: mix_send.at[peer], mix_recv.at[kv], 1)

    def send_back(peer):
        @pl.when(lax.rem(peer + kv_peers - 1, kv_peers) < rank)
        def _():
            send_mix(peer)

    def send_on(peer):
        pl.semaphore_wait(ready_sems.at[peer], 1)
        send_mix(peer)

    with jax.named_scope("fan_mix"):
        far_first(kv_peers, kv, send_back)
        loop(rank + 1, kv_peers, lambda which: send_on(at_rank(which)))
    own_folded[...] = folded(block)

    with jax.named_scope("mix_wait"):
        wait_bytes(mix_recv, kv_peers - 1, recv_sems.at[1])
    mix = summed(mix_recv)
    small_at = 4 * head_dim
    scale = lax.rsqrt(mix[:, small_at + 2 : small_at + 3] / features + EPSILON)
    query_raw = mix[:, 0:head_dim] * scale
    key_raw = mix[:, head_dim : 2 * head_dim] * scale
    value_vec = mix[:, 2 * head_dim : 3 * head_dim] * scale
    z_gate = mix[:, 3 * head_dim : 4 * head_dim] * scale
    decay_pre = mix[:, small_at : small_at + 1] * scale
    beta_gate = jax.nn.sigmoid(mix[:, small_at + 1 : small_at + 2] * scale)

    def unit(values):
        return values * lax.rsqrt(jnp.sum(values * values, axis=1, keepdims=True) + EPSILON)

    query = unit(query_raw) * head_dim ** (-0.5)
    key_vec = unit(key_raw)
    softplus = jnp.maximum(decay_pre, 0.0) + jnp.log1p(jnp.exp(-jnp.abs(decay_pre)))
    decay = jnp.exp(-decay_rate[...].reshape(1, 1) * softplus)
    columns = jnp.concatenate([key_vec, query], axis=0).T
    recalled = []
    looked_up = []
    for at in range(seqs):
        one = state[at]
        recalled.append(jnp.sum(one * columns[:, at : at + 1], axis=0, keepdims=True))
        looked_up.append(jnp.sum(one * columns[:, seqs + at : seqs + at + 1], axis=0, keepdims=True))
    recalled = jnp.concatenate(recalled, axis=0) * decay
    looked_up = jnp.concatenate(looked_up, axis=0) * decay
    update = beta_gate * (value_vec - recalled)
    head_out = looked_up + update * jnp.sum(key_vec * query, axis=1, keepdims=True)
    gain = head_gain[...].reshape(1, head_dim)
    mixed = head_out * lax.rsqrt(jnp.mean(head_out * head_out, axis=1, keepdims=True) + EPSILON)
    mixed = (mixed * gain * silu(z_gate)).astype(BF16)
    head_slots[kv] = mixed
    with jax.named_scope("fan_heads"):
        far_first(kv_peers, kv, copy_to("kv", lambda peer: head_slots.at[kv], head_slots.at[kv], 2))

    for at in range(seqs):
        new_state_ref[at] = decay[at : at + 1] * state[at] + columns[:, at : at + 1] * update[at : at + 1]

    with jax.named_scope("heads_wait"):
        wait_bytes(head_slots, kv_peers - 1, recv_sems.at[2])
    attn = folded(dot(merge_rows(head_slots), w_out[...]))
    out_send[...] = attn.reshape(out_send.shape).astype(BF16)
    piece = lax.rem(tp, pieces_count)
    out_recv[tp] = out_send[piece]
    with jax.named_scope("fan_out"):
        far_first(
            tp_peers, tp, copy_to("tp", lambda peer: out_send.at[lax.rem(peer, pieces_count)], out_recv.at[tp], 3)
        )
    with jax.named_scope("out_wait"):
        wait_bytes(out_recv, tp_peers - 1, recv_sems.at[3])
    piece_rows = out_send.shape[1]
    own_piece = own_folded[pl.ds(pl.multiple_of(piece * piece_rows, piece_rows), piece_rows)]
    resid_slots[piece] = (own_piece + summed(out_recv)).astype(BF16)
    send_piece = copy_to("tp", lambda peer: resid_slots.at[piece], resid_slots.at[piece], 4)
    with jax.named_scope("fan_resid"):
        for offset in sorted(range(-(window // 2), window - window // 2), key=lambda offset: -abs(offset)):
            if offset:
                send_piece(on_chip(offset, 0))
                send_piece(on_chip(offset, 1))
        send_piece(on_chip(0, 1 - core))

    with jax.named_scope("resid_wait"):
        wait_bytes(resid_slots, pieces_count - 1, recv_sems.at[4])
    resid = resid_slots[...].astype(F32).reshape(fold, 2 * batch)
    normed, squares = normed_block(unfolded(resid), mlp_gain)
    pieces = dot_rows(normed, w_hidden[...])
    piece_lane = lax.broadcasted_iota(jnp.int32, pieces.shape, 1)
    pieces = jnp.where(piece_lane == ff, squares, pieces)
    to_sequences(pieces, hidden_send, hidden_recv)
    with jax.named_scope("fan_hidden"):
        far_first(kv_peers, kv, copy_to("kv", lambda peer: hidden_send.at[peer], hidden_recv.at[kv], 5))
    resid_folded[...] = resid

    with jax.named_scope("hidden_wait"):
        wait_bytes(hidden_recv, kv_peers - 1, recv_sems.at[5])
    both = summed(hidden_recv)
    scale = lax.rsqrt(both[:, ff : ff + 1] / features + EPSILON)
    hidden = silu(both[:, :ff_pad] * scale) * (both[:, ff_pad:] * scale)
    hidden_slots[kv] = hidden.astype(BF16)
    with jax.named_scope("fan_act"):
        far_first(kv_peers, kv, copy_to("kv", lambda peer: hidden_slots.at[kv], hidden_slots.at[kv], 6))

    with jax.named_scope("act_wait"):
        wait_bytes(hidden_slots, kv_peers - 1, recv_sems.at[6])
    down = folded(dot(merge_rows(hidden_slots), w_down_split[...]))
    for at in range(tp_peers):
        down_send[at] = down[at * part : (at + 1) * part].astype(BF16)
    down_recv[tp] = down_send[tp]
    with jax.named_scope("fan_down"):
        far_first(tp_peers, tp, copy_to("tp", lambda peer: down_send.at[peer], down_recv.at[tp], 7))
    own_at = tp * width
    own_rows = resid_folded[pl.ds(pl.multiple_of(lax.rem(own_at, fold), width), width)]
    own_rows = jnp.where(own_at >= fold, own_rows[:, batch:], own_rows[:, :batch])
    with jax.named_scope("down_wait"):
        wait_bytes(down_recv, tp_peers - 1, recv_sems.at[7])
    total = summed(down_recv)
    total = jnp.concatenate([total[:, :batch], total[:, batch:]], axis=0)
    next_ref[...] = (own_rows + total).astype(BF16)

    with jax.named_scope("sends"):
        for slots, count, phase in (
            (gathered, 4 * near + 1, 0),
            (gathered, 4 * near - 2, 8),
            (mix_send, kv_peers - 1, 1),
            (head_slots, kv_peers - 1, 2),
            (out_recv, tp_peers - 1, 3),
            (resid_slots, pieces_count - 1, 4),
            (hidden_send, kv_peers - 1, 5),
            (hidden_slots, kv_peers - 1, 6),
            (down_send, tp_peers - 1, 7),
        ):
            wait_bytes(slots, count, send_sems.at[phase])


def local(
    kv_peers,
    tp_peers,
    stream,
    attn_gain,
    mlp_gain,
    w_query,
    w_key,
    w_value,
    w_zgate,
    w_decay,
    w_beta,
    decay_rate,
    head_gain,
    w_attn_out,
    w_gate,
    w_up,
    w_down,
    state,
):
    batch, width = stream.shape
    rows, head_dim = w_query.shape
    seqs = state.shape[0]
    heads = w_decay.shape[1]
    ff = w_gate.shape[1]
    ff_pad = pl.cdiv(ff + 1, LANES) * LANES
    vmem = pl.BlockSpec(memory_space=pltpu.VMEM)
    hbm = pl.BlockSpec(memory_space=pl.ANY)
    pieces = tp_peers // REPEATS
    piece_slots = (rows // 2 // pieces, 2 * batch)
    down_slots = pltpu.VMEM((tp_peers, width // 2, 2 * batch), BF16)
    mix_slots = pltpu.VMEM((kv_peers, seqs, 4 * head_dim + LANES), BF16)
    hidden_slots = pltpu.VMEM((kv_peers, seqs, 2 * ff_pad), BF16)
    next_stream, new_state = pl.pallas_call(
        functools.partial(layer, kv_peers, tp_peers),
        name="layer",
        out_shape=(
            pltpu.VMEM((width, batch), BF16),
            pltpu.VMEM((seqs, head_dim, head_dim), F32),
        ),
        in_specs=[hbm] * 16,
        out_specs=(vmem, vmem),
        scratch_shapes=[
            pltpu.VMEM(attn_gain.shape, BF16),
            pltpu.VMEM(mlp_gain.shape, BF16),
            pltpu.VMEM(decay_rate.shape, F32),
            pltpu.VMEM(head_gain.shape, F32),
            pltpu.VMEM((rows, 4 * head_dim + LANES), BF16),
            pltpu.VMEM((2, heads, rows), BF16),
            pltpu.VMEM((head_dim, w_attn_out.shape[1]), BF16),
            pltpu.VMEM((2 * ff_pad, rows), BF16),
            pltpu.VMEM((ff_pad, rows), BF16),
            pltpu.VMEM((ff_pad, rows), BF16),
            pltpu.VMEM((seqs, head_dim, head_dim), F32),
            pltpu.VMEM((rows // 2, 2 * batch), F32),
            pltpu.VMEM((rows // 2, 2 * batch), F32),
            pltpu.VMEM((tp_peers, width, batch), BF16),
            mix_slots,
            mix_slots,
            pltpu.VMEM((kv_peers, seqs, head_dim), BF16),
            pltpu.VMEM((pieces, *piece_slots), BF16),
            pltpu.VMEM((tp_peers, *piece_slots), BF16),
            pltpu.VMEM((pieces, *piece_slots), BF16),
            hidden_slots,
            hidden_slots,
            pltpu.VMEM((kv_peers, seqs, ff_pad), BF16),
            down_slots,
            down_slots,
            pltpu.SemaphoreType.DMA,
            pltpu.SemaphoreType.DMA((tp_peers,)),
            pltpu.SemaphoreType.DMA((15,)),
            pltpu.SemaphoreType.REGULAR((kv_peers,)),
            pltpu.SemaphoreType.REGULAR((tp_peers,)),
            pltpu.SemaphoreType.DMA((9,)),
            pltpu.SemaphoreType.DMA((9,)),
        ],
        compiler_params=pltpu.CompilerParams(collective_id=0, has_side_effects=True),
    )(
        stream.T,
        attn_gain,
        mlp_gain,
        decay_rate,
        head_gain,
        w_query,
        w_key,
        w_value,
        w_zgate,
        w_decay.T,
        w_beta.T,
        w_attn_out,
        w_gate.T,
        w_up.T,
        w_down,
        state.reshape(seqs, head_dim, head_dim),
    )
    return next_stream.T, new_state.reshape(state.shape)


def solution(mesh):
    return jax.shard_map(
        functools.partial(local, mesh.shape["kv"], mesh.shape["tp"]),
        mesh=mesh,
        in_specs=(
            P("grp", ("kv", "tp")),
            P("kv"),
            P("kv"),
            P("kv", "tp"),
            P("kv", "tp"),
            P("kv", "tp"),
            P("kv", "tp"),
            P("kv", None),
            P("kv", None),
            P("tp"),
            P(),
            P("tp", "kv"),
            P("kv", "tp"),
            P("kv", "tp"),
            P("tp", "kv"),
            P(("grp", "kv"), "tp", None, None),
        ),
        out_specs=(P("grp", ("kv", "tp")), P(("grp", "kv"), "tp", None, None)),
        check_vma=False,
    )
```
